32 devices in a mesh: fs: 8 (over z, y), tp: 4 (over x, core).
Axes of the slice: x: 2, y: 2, z: 4, core: 2. Of those that a mesh axis runs over, the one named last changes fastest.
Arguments:
- prompt: bfloat16 [4096, 4096], P('fs'), may hold values from -6 to 6
- expert_ids: int32 [4096, 2], P('fs'), may hold values from 0 to 15, all different within a row; in each aligned block of 512 rows (0 to 511, 512 to 1023, ...) at most 96 rows name the same one
- group_weight: float32 [4096], P('fs'), may hold values from 0.25 to 1
- expert_share: float32 [4096, 2], P('fs'), may hold values from 0.1 to 1
- norm_gain: float32 [4096], P('fs'), may hold values from 0.1 to 1.9
- gate_train: float32 [16, 4096, 1024], P(None, 'fs', 'tp'), may hold values from -0.09375 to 0.09375
- up_train: float32 [16, 4096, 1024], P(None, 'fs', 'tp'), may hold values from -0.09375 to 0.09375
- down_train: float32 [16, 1024, 4096], P(None, 'fs', 'tp'), may hold values from -0.1875 to 0.1875
Outputs:
- mixed: bfloat16 [4096, 4096], P('fs', 'tp')
- gate_new: bfloat16 [16, 4096, 1024], P('fs', None, 'tp')
- up_new: bfloat16 [16, 4096, 1024], P('fs', None, 'tp')
- down_new: bfloat16 [16, 1024, 4096], P('fs', 'tp')
The draws below stay inside these ranges and needn't reach their ends.
Inputs may be any that keep to these rules, and one draw needn't show every extreme that they name: `expert_ids`: each row names two different experts; within the rows of one index of fs no expert is named more than 96 times, a bound that some block reaches there.
All inputs are finite; a program needn't handle non-finite values.
Results may differ from the reference program's by a relative error of at most 0.0086.
Values may be sent and summed in bfloat16 or wider, within the bound.
No kernel may reach another device: no remote copies, remote signals or barrier semaphores. Data moves between devices by JAX's collectives and lax.ppermute only.
A program may use at most 128 MiB of HBM per device.

```python
import math
import jax
import jax.numpy as jnp
import numpy as np
from jax import lax

D = 4096
FF = 1024
TOK_DEV = 512
EXPERTS = 16
TOKENS = 4096
CAP = 96
N_FS = 8


def levels(rng, extent, cuts, smallest, largest):
    gain = 1.0
    for position, shards_of in cuts:
        draws = jax.random.uniform(jax.random.fold_in(jax.random.fold_in(rng, 6), position), (shards_of,), jnp.float32, smallest / len(cuts), largest / len(cuts))
        gain = gain * jnp.repeat(jnp.exp(draws), extent[position] // shards_of).reshape((-1,) + (1,) * (len(extent) - 1 - position))
    return gain


def shared_out(rng, own, number, rows, count, top, most, skew):
    ranking = jax.random.permutation(rng, count)
    packed, ordinary = portions_of(count, rows * top, most, skew, True), portions_of(count, rows * top, most, skew, False)
    places = jnp.arange(count)

    def named(lengths, offset_by):
        used = int((lengths > 0).sum())
        fixed = max(1, used // 4)
        moved = fixed + (places - fixed + offset_by * (used - fixed)) % max(1, count - fixed)
        return jnp.zeros((count,), jnp.int32).at[ranking[jnp.where(places < fixed, places, moved)]].set(jnp.asarray(lengths, jnp.int32))

    lengths = jnp.where(number % 4 == 0, named(packed, number // 4), named(ordinary, number - number // 4 - 1))
    mixed = jax.random.permutation(jax.random.fold_in(own, 3), count)
    giver, sink = mixed[0:count // 2 * 2:2], mixed[1:count // 2 * 2:2]
    slack = jnp.minimum(lengths[giver] - 1, most - lengths[sink]) // 2
    slack = jnp.where((giver == ranking[0]) | (sink == ranking[0]) | (lengths[sink] == 0), 0, jnp.maximum(slack, 0))
    moved = jax.random.randint(jax.random.fold_in(own, 4), (count // 2,), 0, 1 << 20) % (slack + 1)
    lengths = lengths.at[giver].add(-moved).at[sink].add(moved)
    items = jnp.searchsorted(jnp.cumsum(lengths), jnp.arange(rows * top), side="right").astype(jnp.int32)
    grid = items.reshape(top, rows).T
    grid = grid[jax.random.permutation(jax.random.fold_in(own, 1), rows)]
    offset_by = jax.random.randint(jax.random.fold_in(own, 2), (rows, 1), 0, top)
    return jnp.take_along_axis(grid, (jnp.arange(top)[None, :] + offset_by) % top, axis=1)


def portions_of(count, total, reach, skew, full):
    portions = [(1 << 20) // math.isqrt(grade ** skew) + 1 for grade in range(1, count + 1)]
    largest = reach if full else min(reach, max(-(-total // count), total * portions[0] // sum(portions)))
    least = 1 if total - largest >= count - 1 else 0
    counts, spare = [largest] + [least] * (count - 1), total - largest - least * (count - 1)
    while spare > 0:
        candidates = [i for i in range(1, count) if counts[i] < largest] or [i for i in range(1, count) if counts[i] < reach]
        pool, remaining = sum([portions[i] for i in candidates]), spare
        for i in candidates:
            addition = min(reach - counts[i], max(1, remaining * portions[i] // pool), spare)
            counts[i] = counts[i] + addition
            spare = spare - addition
    return np.array(counts)


def bell_draw(rng, shape, spread, most, split=(), kind=jnp.bfloat16):
    array = spread * jax.random.normal(rng, shape, jnp.float32)
    if split:
        array = array * levels(rng, shape, split, -0.22, 0.18)
    return jnp.clip(array, -most, most).astype(kind)


def setup_inputs(seed: int = 0) -> dict:
    key_list = jax.random.split(jax.random.key(seed), 9)
    prompt = bell_draw(key_list[0], (TOKENS, D), 1.0, 6.0, ((0, 8),))
    expert_ids_keys = jax.random.split(jax.random.fold_in(key_list[1], 1), TOKENS // TOK_DEV)
    expert_ids_turns = jax.random.permutation(jax.random.fold_in(key_list[1], 3), TOKENS // TOK_DEV)
    expert_ids = jax.vmap(lambda own, number: shared_out(jax.random.fold_in(key_list[1], 2), own, number, TOK_DEV, EXPERTS, 2, CAP, 1))(expert_ids_keys, expert_ids_turns).reshape((TOKENS, 2))
    group_weight = jnp.clip(jnp.exp(math.log(1.0) - 1.3862944 * jax.random.uniform(key_list[2], (TOKENS,), jnp.float32) ** levels(key_list[2], (TOKENS,), ((0, 8),), -0.2, 0.2)), 0.25, 1.0)
    expert_share = jnp.clip(jnp.exp(math.log(1.0) - 2.3025851 * jax.random.uniform(key_list[3], (TOKENS, 2), jnp.float32) ** levels(key_list[3], (TOKENS, 2), ((0, 8),), -0.2, 0.2)), 0.1, 1.0)
    norm_gain = jnp.clip(1.0 + 0.18 * jax.random.normal(key_list[4], (D,), jnp.float32), 0.1, 1.9)
    gate_train = bell_draw(key_list[5], (EXPERTS, D, FF), D ** -0.5, 0.09375, ((1, 8), (2, 4)), jnp.float32)
    up_train = bell_draw(key_list[6], (EXPERTS, D, FF), D ** -0.5, 0.09375, ((1, 8), (2, 4)), jnp.float32)
    down_train = bell_draw(key_list[7], (EXPERTS, FF, D), FF ** -0.5, 0.1875, ((1, 8), (2, 4)), jnp.float32)
    return dict(prompt=prompt, expert_ids=expert_ids, group_weight=group_weight, expert_share=expert_share, norm_gain=norm_gain, gate_train=gate_train, up_train=up_train, down_train=down_train)


EPS = 1e-06

def reference(prompt, expert_ids, group_weight, expert_share, norm_gain, gate_train, up_train, down_train):
    gain_rows = norm_gain[None, :, None]
    gate_new = (gate_train * gain_rows).astype(jnp.bfloat16)
    up_new = (up_train * gain_rows).astype(jnp.bfloat16)
    down_new = down_train.astype(jnp.bfloat16)
    widened = prompt.astype(jnp.float32)
    normed = (widened * lax.rsqrt(lax.optimization_barrier(jnp.mean(widened * widened, axis=-1, keepdims=True)) + EPS)).astype(jnp.bfloat16)
    blocks = expert_ids.reshape(N_FS, TOK_DEV * 2)
    onehot = (blocks[:, :, None] == jnp.arange(EXPERTS, dtype=jnp.int32)[None, None, :]).astype(jnp.int32)
    slot_rank = lax.optimization_barrier(jnp.sum((jnp.cumsum(onehot, axis=1) - 1) * onehot, axis=2))
    slots = (jnp.arange(N_FS, dtype=jnp.int32)[:, None] * CAP + slot_rank).reshape(TOKENS, 2).astype(jnp.int32)
    token_rows = jnp.broadcast_to(normed[:, None, :], (TOKENS, 2, D))
    buffer = jnp.zeros((EXPERTS, N_FS * CAP, D), jnp.bfloat16).at[expert_ids, slots].set(token_rows)

    def expert(operands):
        expert_rows, w_gate, w_up, w_down = operands
        gate_val = jnp.dot(expert_rows, w_gate, preferred_element_type=jnp.float32)
        up_val = jnp.dot(expert_rows, w_up, preferred_element_type=jnp.float32)
        hidden = (jax.nn.silu(gate_val) * up_val).astype(jnp.bfloat16)
        return jnp.dot(hidden, w_down, preferred_element_type=jnp.float32).astype(jnp.bfloat16)
    outputs = lax.map(expert, (buffer, gate_new, up_new, down_new))
    picked = outputs[expert_ids, slots].astype(jnp.float32)
    weights = group_weight[:, None] * expert_share / lax.optimization_barrier(jnp.sum(expert_share, axis=1, keepdims=True))
    mixed = lax.optimization_barrier(jnp.sum(weights[:, :, None] * picked, axis=1)).astype(jnp.bfloat16)
    return (mixed, gate_new, up_new, down_new)
```

```python
import jax
import jax.numpy as jnp
from jax import lax
from jax.experimental import pallas as pl
from jax.experimental.pallas import tpu as pltpu
from jax.sharding import PartitionSpec as P


EPS = 1e-06
BF = jnp.bfloat16
F32 = jnp.float32


def mark():
    def body(in_ref, out_ref):
        out_ref[...] = in_ref[...]

    pl.pallas_call(
        body,
        out_shape=jax.ShapeDtypeStruct((8, 128), F32),
        compiler_params=pltpu.CompilerParams(has_side_effects=True),
    )(jnp.zeros((8, 128), F32))


def swap(value, axis, bits):
    size = lax.axis_size(axis)
    return lax.ppermute(value, axis, [(i, i ^ bits) for i in range(size)])


def cut(value, start, size, axis):
    return lax.dynamic_slice_in_dim(value, start, size, axis, allow_negative_indices=False)


def tied(values, anchor):
    return lax.optimization_barrier((values, anchor))[0]


def spread(value):
    pieces = {0: value}
    bit = lax.axis_size("tp") // 2
    while bit:
        for distance, piece in list(pieces.items()):
            pieces[distance ^ bit] = swap(piece, "tp", bit)
        bit //= 2
    return pieces


def whole_vmem(count):
    return [pl.BlockSpec(memory_space=pltpu.VMEM)] * count


def combine(weights, blocks, total, dtype):
    tokens, slots = weights.shape
    cap, width = blocks[0].shape
    count = len(blocks)
    tile = min(256, width)

    def body(weights_ref, *refs):
        block_refs, refs = refs[:count], refs[count:]
        total_ref = None if total is None else refs[0]
        out_ref, whole = refs[-2], refs[-1]
        for q in range(count):
            whole[q * cap : (q + 1) * cap, :] = block_refs[q][...]

        @pl.loop(0, width // tile)
        def _(i):
            columns = pl.ds(pl.multiple_of(i * tile, tile), tile)
            term = jnp.dot(weights_ref[...], whole[:, columns], preferred_element_type=F32)
            if total_ref is not None:
                term = term + total_ref[:, columns]
            out_ref[:, columns] = term.astype(dtype)

    operands = [weights, *blocks] + ([] if total is None else [total])
    return pl.pallas_call(
        body,
        out_shape=jax.ShapeDtypeStruct((tokens, width), dtype),
        in_specs=whole_vmem(len(operands)),
        out_specs=whole_vmem(1)[0],
        scratch_shapes=[pltpu.VMEM((slots, width), BF)],
        cost_estimate=pl.CostEstimate(
            flops=2 * tokens * slots * width, bytes_accessed=2 * slots * width, transcendentals=0
        ),
    )(*operands)


def project(places, blocks, rows, gate=None):
    local, depth, cols = blocks[0].shape
    count = len(blocks)
    groups, parts = len(rows), len(rows[0])
    height, piece = rows[0][0].shape[1:]
    order = [m for m in sorted(rows[0])]
    flat = [group[m] for group in rows for m in order]

    def body(places_ref, *refs):
        block_refs, refs = refs[:count], refs[count:]
        row_refs, refs = refs[: len(flat)], refs[len(flat) :]
        gate_ref = None if gate is None else refs[0]
        whole_ref, out_ref = refs[-2:]
        me, tp = places_ref[0], places_ref[1]
        for k in range(count):
            spot = pl.ds(pl.multiple_of((me ^ k) * depth, depth), depth)
            whole_ref[0, spot, :] = block_refs[k][0]
        for g in range(groups):
            total = None
            for i, m in enumerate(order):
                spot = pl.ds(pl.multiple_of((tp ^ m) * piece, piece), piece)
                term = jnp.dot(
                    row_refs[g * parts + i][0],
                    whole_ref[0, spot, :],
                    preferred_element_type=F32,
                )
                total = term if total is None else total + term
            spot = slice(g * height, (g + 1) * height)
            if gate_ref is not None:
                value = gate_ref[0, spot, :]
                total = (value / (1.0 + jnp.exp(-value))) * total
            out_ref[0, spot, :] = total.astype(out_ref.dtype)

    def spec(*shape):
        return pl.BlockSpec((1,) + shape, lambda e, places: (e, 0, 0))

    many = groups * height
    return pl.pallas_call(
        body,
        grid_spec=pltpu.PrefetchScalarGridSpec(
            num_scalar_prefetch=1,
            grid=(local,),
            in_specs=[spec(depth, cols)] * count
            + [spec(height, piece)] * len(flat)
            + ([] if gate is None else [spec(many, cols)]),
            out_specs=[spec(depth * count, cols), spec(many, cols)],
        ),
        out_shape=[
            jax.ShapeDtypeStruct((local, depth * count, cols), BF),
            jax.ShapeDtypeStruct((local, many, cols), F32 if gate is None else BF),
        ],
        compiler_params=pltpu.CompilerParams(vmem_limit_bytes=48 << 20),
        cost_estimate=pl.CostEstimate(
            flops=2 * local * many * cols * piece * parts,
            bytes_accessed=4 * local * (depth * count * cols + many * piece),
            transcendentals=0,
        ),
    )(places, *blocks, *flat, *([] if gate is None else [gate]))


def lower(places, blocks, hidden, l, cap):
    depth, cols = blocks[0].shape
    count = len(blocks)
    order = [m for m in sorted(hidden)]
    parts = len(order)
    many, part = hidden[0].shape[1:]
    tile = min(256, cols)

    def body(places_ref, *refs):
        block_refs, refs = refs[:count], refs[count:]
        hidden_refs, refs = refs[:parts], refs[parts:]
        out_refs, refs = refs[:count], refs[count:]
        part_refs, whole = refs[:parts], refs[-1]
        me, tp = places_ref[0], places_ref[1]
        for k in range(count):
            spot = pl.ds(pl.multiple_of((me ^ k) * depth, depth), depth)
            whole[spot, :] = block_refs[k][...]

        @pl.loop(0, cols // tile)
        def _(i):
            columns = pl.ds(pl.multiple_of(i * tile, tile), tile)
            total = None
            for j, m in enumerate(order):
                spot = pl.ds(pl.multiple_of((tp ^ m) * part, part), part)
                weight = whole[spot, columns]
                part_refs[j][:, columns] = weight
                term = jnp.dot(hidden_refs[j][...], weight, preferred_element_type=F32)
                total = term if total is None else total + term
            total = total.astype(BF)
            for q in range(count):
                out_refs[q][:, columns] = total[q * cap : (q + 1) * cap]

    vmem = whole_vmem(1)[0]
    results = pl.pallas_call(
        body,
        in_specs=[pl.BlockSpec(memory_space=pltpu.SMEM)] + whole_vmem(count + parts),
        out_specs=[vmem] * (count + parts),
        out_shape=[jax.ShapeDtypeStruct((cap, cols), BF)] * count
        + [jax.ShapeDtypeStruct((part, cols), BF)] * parts,
        scratch_shapes=[pltpu.VMEM((depth * count, cols), BF)],
        compiler_params=pltpu.CompilerParams(vmem_limit_bytes=48 << 20),
        cost_estimate=pl.CostEstimate(
            flops=2 * many * cols * depth * count,
            bytes_accessed=4 * depth * count * cols,
            transcendentals=0,
        ),
    )(places, *blocks, *[hidden[m][l] for m in order])
    return results[:count], dict(zip(order, results[count:]))


def on_device(
    prompt, expert_ids, group_weight, expert_share, norm_gain, gate_train, up_train, down_train
):
    n = lax.axis_size("fs")
    parts = lax.axis_size("tp")
    me = lax.axis_index("fs")
    tp = lax.axis_index("tp")
    tokens, width = prompt.shape
    experts = gate_train.shape[0]
    local = experts // n
    cap = max(2, 3 * tokens // experts)
    half = n // 2
    piece = width // parts
    hidden_part = gate_train.shape[2]
    gain = norm_gain[None, :, None]

    def block(weights, k, scale=None):
        picked = cut(weights, (me ^ k) * local, local, 0)
        if scale is not None:
            picked = picked * scale
        return picked.astype(BF)

    near = list(range(1, half))
    far = list(range(half, n))

    ids = expert_ids.T
    expert_row = lax.broadcasted_iota(jnp.int32, (experts, tokens), 0)
    named = [ids[k][None, :] == expert_row for k in range(2)]
    chosen = named[0] | named[1]
    before = (
        lax.broadcasted_iota(jnp.int32, (tokens, tokens), 0)
        < lax.broadcasted_iota(jnp.int32, (tokens, tokens), 1)
    ).astype(BF)
    count = jnp.dot(chosen.astype(BF), before, preferred_element_type=F32)
    rank = jnp.where(chosen, count, -1.0).astype(BF)
    rank_other = swap(rank, "fs", half)

    wide = prompt.astype(F32)
    scale = lax.rsqrt(jnp.mean(wide * wide, axis=-1, keepdims=True) + EPS)
    own = cut(prompt, tp * piece, piece, 1)
    own = (own.astype(F32) * scale).astype(BF)
    other = swap(own, "fs", half)

    slot_row = lax.broadcasted_iota(jnp.int32, (1, cap, 1), 1).astype(BF)

    def pick(ranks, values, j):
        rows = cut(ranks, (me ^ j) * local, local, 0)
        mask = (rows[:, None, :] == slot_row).astype(BF).reshape(local * cap, tokens)
        got = jnp.dot(mask, values, preferred_element_type=F32).astype(BF)
        return got.reshape(local, cap, piece)

    places = jnp.stack([me, tp]).astype(jnp.int32)

    def route(ranks, values):
        got = [pick(ranks, values, j) for j in range(half)]
        rows = [swap(got[j], "fs", j) if j else got[0] for j in range(half)]
        return jnp.concatenate(rows, axis=1), got[half - 1]

    rows_a, _ = route(rank, own)
    gate_got = {k: block(gate_train, k, gain) for k in range(n)}
    for k in near:
        gate_got[k] = swap(gate_got[k], "fs", k)
    for k in far[:1]:
        gate_got[k] = swap(gate_got[k], "fs", k)
    mark()

    rows_b, anchor = route(rank_other, other)
    for k in far[1:]:
        gate_got[k] = swap(tied(gate_got[k], anchor), "fs", k)
    rows = [spread(rows_a)]
    mark()

    rows.append(spread(rows_b))
    up_got = {k: tied(block(up_train, k, gain), rows_b) for k in range(n)}
    for k in far + near:
        up_got[k] = swap(up_got[k], "fs", k)
    mark()

    def bring(l, anchor):
        got = {}
        for k in [0] + far + near:
            part = tied(cut(down_train, (me ^ k) * local + l, 1, 0)[0].astype(BF), anchor)
            got[k] = swap(part, "fs", k) if k else part
        return [got[k] for k in range(n)]

    down_got = [bring(l, rows[1][parts // 2]) for l in range(local - 1)]
    mark()

    gate_new, gate_val = project(places, [gate_got[k] for k in range(n)], rows)
    up_new, hidden = project(places, [up_got[k] for k in range(n)], rows, gate_val)
    down_got.append(bring(local - 1, gate_val))
    hidden_by = spread(hidden)
    mark()

    share = group_weight[:, None] * expert_share / jnp.sum(expert_share, axis=1, keepdims=True)
    share = share.T
    weight = jnp.where(named[0], share[0][None, :], 0.0) + jnp.where(
        named[1], share[1][None, :], 0.0
    )
    column = lax.broadcasted_iota(jnp.int32, (experts, n * cap), 1)
    row = lax.broadcasted_iota(jnp.int32, (experts, n * cap), 0)
    slot_col = (lax.broadcasted_iota(jnp.int32, (tokens, n * cap), 1) % cap).astype(F32)

    def combiner(l):
        expand = (row == (me ^ (column // cap)) * local + l).astype(BF)
        contract = (((0,), (0,)), ((), ()))
        ranks = lax.dot_general(rank, expand, contract, preferred_element_type=F32)
        weights = lax.dot_general(
            weight.astype(BF), expand, contract, preferred_element_type=F32
        )
        return jnp.where(ranks == slot_col, weights, 0.0).astype(BF)

    total = None
    down_new = jnp.zeros((local, hidden_part, width), BF)
    for l in range(local):
        last = l == local - 1
        out, sent = lower(places, down_got[l], hidden_by, l, cap)
        back = {}
        for q in [0] + far + near:
            back[q] = swap(out[q], "fs", q) if q else out[q]
        for m in range(1, parts):
            sent[m] = swap(sent[m], "tp", m)
        mark()
        for m in range(parts):
            down_new = lax.dynamic_update_slice(
                down_new,
                sent[m][None],
                (l, 0, (tp ^ m) * piece),
                allow_negative_indices=False,
            )
        total = combine(
            combiner(l), [back[q] for q in range(n)], total, BF if last else F32
        )
    return (total, gate_new, up_new, down_new)


def solution(mesh):
    placed = (
        P("fs", None),
        P("fs", None),
        P("fs"),
        P("fs", None),
        P("fs"),
        P(None, "fs", "tp"),
        P(None, "fs", "tp"),
        P(None, "fs", "tp"),
    )
    return jax.shard_map(
        on_device,
        mesh=mesh,
        in_specs=placed,
        out_specs=(P("fs", "tp"), P("fs", None, "tp"), P("fs", None, "tp"), P("fs", "tp", None)),
        check_vma=False,
    )
```
